32 devices in a mesh: grp: 2 (over y), sp: 4 (over z), tp: 4 (over x, core).
Axes of the slice: x: 2, y: 2, z: 4, core: 2. Of those that a mesh axis runs over, the one named last changes fastest.
Arguments:
- queries: bfloat16 [6144, 512], P(('grp', 'sp'), 'tp'), parts along dimension 0, may hold values from -6 to 6
- key_projected: bfloat16 [6144, 512], P(('grp', 'sp'), 'tp'), parts along dimension 0, may hold values from -6 to 6
- values: bfloat16 [6144, 1024], P(('grp', 'sp'), 'tp'), parts along dimension 0, may hold values from -6 to 6
- output_gate_preact: bfloat16 [6144, 1024], P(('grp', 'sp'), 'tp'), parts along dimension 0, may hold values from -6 to 6
- forward_decay_logits: bfloat16 [6144, 512], P(('grp', 'sp'), 'tp'), parts along dimension 0, may hold values from -3.8 to 3.8
- backward_decay_logits: bfloat16 [6144, 512], P(('grp', 'sp'), 'tp'), parts along dimension 0, may hold values from -3.8 to 3.8
- decay_logit_shift: float32 [2, 512], P(None, 'tp'), may hold values from -1 to 13
- decay_spike_values: float32 [8, 6144], P('tp', ('grp', 'sp')), parts along dimension 1, may hold values from -2.1 to 0
- residual: bfloat16 [6144, 2048], P(('grp', 'sp', 'tp')), parts along dimension 0, may hold values from -6 to 6
- head_norm_gain: float32 [1024], P('tp'), may hold values from 0.1 to 1.9
- output_projection: bfloat16 [1024, 2048], P('tp'), may hold values from -0.1875 to 0.1875
- prenorm_gain: float32 [2048], replicated, may hold values from 0.1 to 1.9
- gate_projection: bfloat16 [2048, 5120], P('sp', 'tp'), may hold values from -0.125 to 0.125
- up_projection: bfloat16 [2048, 5120], P('sp', 'tp'), may hold values from -0.125 to 0.125
- down_projection: bfloat16 [5120, 2048], P('tp', 'sp'), may hold values from -0.078125 to 0.078125
Outputs:
- layer_output: bfloat16 [6144, 2048], P(('grp', 'sp', 'tp')), parts along dimension 0
The draws below stay inside these ranges and needn't reach their ends.
There are 2 independent parts, one for each index of `grp`. The reference program is written for one: setup_inputs(seed, part) draws one part's arguments, and reference() takes and returns one part's arrays. A program takes and returns all parts, laid end to end along the dimension named above; an argument that names none is the same for every part. Nothing has to cross between parts.
All inputs are finite; a program needn't handle non-finite values.
Results may differ from the reference program's by a relative error of at most 0.014.
Values may be sent and summed in bfloat16 or wider, within the bound.
A program may use at most 64 MiB of HBM per device.

```python
import jax
import jax.numpy as jnp
from jax import lax

D = 2048
HEAD_TOTAL = 8
KEY_CHANNELS = 64
HEAD_V = 128
FF = 5120
BLOCK = 64
TOK_DEV = 768
TOKENS = 3072
N_TP = 4


def logit_draw(key):
    noise_key, block_key = jax.random.split(key)
    noise = jnp.clip(0.7 * jax.random.normal(noise_key, (TOKENS, HEAD_TOTAL * KEY_CHANNELS), jnp.float32), -3.0, 3.0)
    shifts = jax.random.uniform(block_key, (TOKENS // TOK_DEV, 1), jnp.float32, -0.8, 0.8)
    return (noise + jnp.repeat(shifts, TOK_DEV, axis=0)).astype(jnp.bfloat16)


def draw_forward_decay_logits(key, part):
    return logit_draw(jax.random.fold_in(key, 11))


def draw_backward_decay_logits(key, part):
    return logit_draw(jax.random.fold_in(key, 12))


def draw_decay_logit_shift(key, part):
    pick_key, slow_key, quick_key = jax.random.split(jax.random.fold_in(key, 13), 3)
    fast_share = 0.5
    fast_heads = jax.random.uniform(pick_key, (2, HEAD_TOTAL), jnp.float32) < fast_share
    fast_channels = jnp.repeat(fast_heads, KEY_CHANNELS, axis=1)
    slow_start = jnp.log(TOKENS / 16.0)
    slow = slow_start + 2.5 * jax.random.uniform(slow_key, (2, HEAD_TOTAL * KEY_CHANNELS), jnp.float32)
    quick = jax.random.uniform(quick_key, (2, HEAD_TOTAL * KEY_CHANNELS), jnp.float32, -1.0, 1.0)
    return jnp.where(fast_channels, quick, slow).astype(jnp.float32)


def draw_decay_spike_values(key, part):
    spot_key, depth_key = jax.random.split(jax.random.fold_in(key, 14))
    spots = jax.random.randint(spot_key, (HEAD_TOTAL, 3), 0, TOKENS)
    depth = jax.random.uniform(depth_key, (HEAD_TOTAL, 3), jnp.float32, -0.69, -0.22)
    places = jnp.arange(TOKENS)[None, None, :] == spots[:, :, None]
    return jnp.sum(jnp.where(places, depth[:, :, None], 0.0), axis=1).astype(jnp.float32)


def block_levels(key, shape, pieces, low, largest):
    def one(position, parts):
        draws = jax.random.uniform(jax.random.fold_in(jax.random.fold_in(key, 6), position), (parts,), jnp.float32, low / len(pieces), largest / len(pieces))
        return jnp.repeat(jnp.exp(draws), shape[position] // parts).reshape((-1,) + (1,) * (len(shape) - position - 1))

    gain = one(*pieces[0])
    for cut in pieces[1:]:
        gain = gain * one(*cut)
    return gain


def gaussian(key, dims, deviation, reach, shards=(), kind=jnp.bfloat16):
    array = deviation * jax.random.normal(key, dims, jnp.float32)
    if shards:
        array = array * block_levels(key, dims, shards, -0.22, 0.18)
    return jnp.clip(array, -reach, reach).astype(kind)


def setup_inputs(seed: int = 0, part: int = 0) -> dict:
    keys = jax.random.split(jax.random.key(seed), 16)
    part_keys = jax.random.split(jax.random.fold_in(keys[15], part), 16)
    queries = gaussian(part_keys[0], (TOKENS, HEAD_TOTAL * KEY_CHANNELS), 1.0, 6.0, ((0, 4), (1, 4)))
    key_projected = gaussian(part_keys[1], (TOKENS, HEAD_TOTAL * KEY_CHANNELS), 1.0, 6.0, ((0, 4), (1, 4)))
    values = gaussian(part_keys[2], (TOKENS, HEAD_TOTAL * HEAD_V), 1.0, 6.0, ((0, 4), (1, 4)))
    output_gate_preact = gaussian(part_keys[3], (TOKENS, HEAD_TOTAL * HEAD_V), 1.0, 6.0, ((0, 4), (1, 4)))
    forward_decay_logits = draw_forward_decay_logits(jax.random.fold_in(jax.random.fold_in(keys[15], part), 71), part)
    backward_decay_logits = draw_backward_decay_logits(jax.random.fold_in(jax.random.fold_in(keys[15], part), 71), part)
    decay_logit_shift = draw_decay_logit_shift(jax.random.fold_in(keys[15], 71), part)
    decay_spike_values = draw_decay_spike_values(jax.random.fold_in(jax.random.fold_in(keys[15], part), 71), part)
    residual = gaussian(part_keys[8], (TOKENS, D), 1.0, 6.0, ((0, 16),))
    head_norm_gain = jnp.clip(1.0 + 0.18 * jax.random.normal(keys[9], (HEAD_TOTAL * HEAD_V,), jnp.float32), 0.1, 1.9)
    output_projection = gaussian(keys[10], (HEAD_TOTAL * HEAD_V, D), (HEAD_TOTAL * HEAD_V) ** -0.5, 0.1875, ((0, 4),))
    prenorm_gain = jnp.clip(1.0 + 0.18 * jax.random.normal(keys[11], (D,), jnp.float32), 0.1, 1.9)
    gate_projection = gaussian(keys[12], (D, FF), D ** -0.5, 0.125, ((0, 4), (1, 4)))
    up_projection = gaussian(keys[13], (D, FF), D ** -0.5, 0.125, ((0, 4), (1, 4)))
    down_projection = gaussian(keys[14], (FF, D), FF ** -0.5, 0.078125, ((0, 4), (1, 4)))
    return dict(queries=queries, key_projected=key_projected, values=values, output_gate_preact=output_gate_preact, forward_decay_logits=forward_decay_logits, backward_decay_logits=backward_decay_logits, decay_logit_shift=decay_logit_shift, decay_spike_values=decay_spike_values, residual=residual, head_norm_gain=head_norm_gain, output_projection=output_projection, prenorm_gain=prenorm_gain, gate_projection=gate_projection, up_projection=up_projection, down_projection=down_projection)


gate_denominator = 16.0
norm_epsilon = 1e-06

def block_sweep(query_in, key_in, values_in, log_decay, span):
    sequence_length, head_count, key_dim = key_in.shape
    block_count = sequence_length // span

    def blocks(tensor):
        return jnp.transpose(tensor.reshape(block_count, span, head_count, tensor.shape[-1]), (0, 2, 1, 3))
    lower_mask = jnp.tril(jnp.ones((span, span), dtype=bool))[:, :, None]

    def advance(carried, inputs):
        memory, offset = carried
        key_blk, value_blk, decay_blk, query_blk = inputs
        within = jnp.cumsum(decay_blk, axis=1)
        ending = within[:, -1, :]
        memory_next = jnp.exp(ending)[:, :, None] * memory + jnp.einsum('hjd,hje->hde', key_blk * jnp.exp(ending[:, None, :] - within), value_blk, precision=lax.Precision.HIGHEST)
        result = jnp.einsum('hid,hde->hie', query_blk * jnp.exp(within), memory, precision=lax.Precision.HIGHEST)
        spread = jnp.exp(jnp.where(lower_mask, within[:, :, None, :] - within[:, None, :, :], -jnp.inf))
        scores = jnp.einsum('hid,hjd,hijd->hij', query_blk, key_blk, spread, precision=lax.Precision.HIGHEST)
        result = result + jnp.einsum('hij,hje->hie', scores, value_blk, precision=lax.Precision.HIGHEST)
        reached = query_blk * jnp.exp(within + offset[:, None, :])
        return ((memory_next, offset + ending), (result, reached))
    start_memory = jnp.zeros((head_count, key_dim, values_in.shape[-1]), jnp.float32)
    start_offset = jnp.zeros((head_count, key_dim), jnp.float32)
    (memory, decay_total), (outputs, reached) = lax.scan(advance, (start_memory, start_offset), (blocks(key_in), blocks(values_in), blocks(log_decay), blocks(query_in)))

    def unblock(tensor):
        return jnp.transpose(tensor, (0, 2, 1, 3)).reshape(sequence_length, head_count, tensor.shape[-1])
    return (unblock(outputs), unblock(reached), memory, decay_total)

def head_mix(combined, head_norm_gain, output_gate_preact):
    sequence_length, head_count, width = combined.shape
    inverse = lax.rsqrt(lax.optimization_barrier(jnp.mean(combined * combined, axis=-1, keepdims=True)) + norm_epsilon)
    gate_act = jax.nn.silu(output_gate_preact.astype(jnp.float32).reshape(sequence_length, head_count, width))
    weighted = combined * inverse * head_norm_gain.reshape(head_count, width) * gate_act
    return weighted.reshape(sequence_length, head_count * width).astype(jnp.bfloat16)

def row_norm(mid_rows, prenorm_gain):
    wide = mid_rows.astype(jnp.float32)
    inverse = lax.rsqrt(lax.optimization_barrier(jnp.mean(wide * wide, axis=-1, keepdims=True)) + norm_epsilon)
    return (wide * inverse * prenorm_gain).astype(jnp.bfloat16)

def reference(queries, key_projected, values, output_gate_preact, forward_decay_logits, backward_decay_logits, decay_logit_shift, decay_spike_values, residual, head_norm_gain, output_projection, prenorm_gain, gate_projection, up_projection, down_projection):
    sequence_length = queries.shape[0]
    query_f = queries.astype(jnp.float32).reshape(sequence_length, HEAD_TOTAL, KEY_CHANNELS) * KEY_CHANNELS ** (-0.5)
    keys_f = key_projected.astype(jnp.float32).reshape(sequence_length, HEAD_TOTAL, KEY_CHANNELS)
    values_f = values.astype(jnp.float32).reshape(sequence_length, HEAD_TOTAL, HEAD_V)
    decay_spikes = jnp.transpose(decay_spike_values)[:, :, None]
    logit_shifts = decay_logit_shift.reshape(2, HEAD_TOTAL, KEY_CHANNELS)
    forward_decay = jax.nn.log_sigmoid(forward_decay_logits.astype(jnp.float32).reshape(sequence_length, HEAD_TOTAL, KEY_CHANNELS) + logit_shifts[0]) / gate_denominator + decay_spikes
    backward_decay = jax.nn.log_sigmoid(backward_decay_logits.astype(jnp.float32).reshape(sequence_length, HEAD_TOTAL, KEY_CHANNELS) + logit_shifts[1]) / gate_denominator + decay_spikes
    fwd_out = block_sweep(query_f, keys_f, values_f, forward_decay, BLOCK)[0]
    bwd_out = block_sweep(query_f[::-1], keys_f[::-1], values_f[::-1], backward_decay[::-1], BLOCK)[0][::-1]
    attended = head_mix(fwd_out + bwd_out, head_norm_gain, output_gate_preact)
    projected = jnp.dot(attended, output_projection, preferred_element_type=jnp.float32)
    mid_rows = (residual.astype(jnp.float32) + projected).astype(jnp.bfloat16)
    normed = row_norm(mid_rows, prenorm_gain)
    gate_part = jnp.dot(normed, gate_projection, preferred_element_type=jnp.float32)
    up_part = jnp.dot(normed, up_projection, preferred_element_type=jnp.float32)
    hidden = (jax.nn.silu(gate_part) * up_part).astype(jnp.bfloat16)
    group_width = FF // N_TP
    summed = jnp.zeros((sequence_length, D), jnp.float32)
    for group_index in range(N_TP):
        low = group_index * group_width
        partial_value = jnp.dot(hidden[:, low:low + group_width], down_projection[low:low + group_width], preferred_element_type=jnp.float32).astype(jnp.bfloat16)
        summed = summed + lax.optimization_barrier(partial_value).astype(jnp.float32)
    return (mid_rows.astype(jnp.float32) + 0.5 * summed).astype(jnp.bfloat16)
```

```python
import functools

import jax
import jax.numpy as jnp
from jax import lax
from jax.experimental import pallas as pl
from jax.experimental.pallas import tpu as pltpu
from jax.sharding import PartitionSpec as P

KEY_CHANNELS = 64
HEAD_V = 128
BLOCK = 64
GATE_DENOMINATOR = 16.0
EPSILON = 1e-06
F32, BF16 = jnp.float32, jnp.bfloat16


def nt(a, b):
    return lax.dot_general(a, b, (((1,), (1,)), ((), ())), preferred_element_type=F32)


def tn(a, b):
    return lax.dot_general(a, b, (((0,), (0,)), ((), ())), preferred_element_type=F32)


def first_head(shape):
    return lax.broadcasted_iota(jnp.int32, shape, 1) < KEY_CHANNELS


def state_kernel(k_ref, v_ref, fd_ref, bd_ref, shift_ref, spike_ref, within_ref, state_ref, kd_ref):
    tokens, lanes = k_ref.shape
    blocks = tokens // BLOCK
    row = lax.broadcasted_iota(jnp.int32, (2 * BLOCK, 2 * BLOCK), 0)
    col = lax.broadcasted_iota(jnp.int32, (2 * BLOCK, 2 * BLOCK), 1)
    r, c = row % BLOCK, col % BLOCK
    ahead = jnp.where(row < BLOCK, r - c, c - r)
    tri = jnp.where(ahead >= 0, 1.0, 0.0).astype(BF16)
    half = first_head((BLOCK, lanes))
    ends = []
    for b in range(blocks):
        at = slice(b * BLOCK, (b + 1) * BLOCK)
        spike = jnp.where(half, spike_ref[at, 0:1], spike_ref[at, 1:2])
        parts = []
        for n, ref in enumerate((fd_ref, bd_ref)):
            x = ref[at, :].astype(F32) + shift_ref[n : n + 1, :]
            soft = jnp.minimum(x, 0.0) - jnp.log1p(jnp.exp(-jnp.abs(x)))
            parts.append(soft / GATE_DENOMINATOR + spike)
        d = jnp.concatenate(parts, axis=1)
        hi = d.astype(BF16)
        lo = (d - hi.astype(F32)).astype(BF16)
        both = jnp.dot(tri, jnp.concatenate([hi, lo], axis=0), preferred_element_type=F32)
        fwd, bwd = both[:BLOCK, :lanes], both[BLOCK:, lanes:]
        within_ref[at, :lanes] = fwd
        within_ref[at, lanes:] = bwd
        ends.append((fwd[BLOCK - 1 :, :], bwd[:1, :]))
    zero = jnp.zeros((1, lanes), F32)
    after, before = [zero] * blocks, [zero] * blocks
    for b in range(1, blocks):
        before[b] = before[b - 1] + ends[b - 1][1]
        after[blocks - 1 - b] = after[blocks - b] + ends[blocks - b][0]
    total_f, total_b = after[0] + ends[0][0], before[-1] + ends[-1][1]
    for b in range(blocks):
        at = slice(b * BLOCK, (b + 1) * BLOCK)
        key = k_ref[at, :].astype(F32)
        kd_ref[at, :lanes] = (key * jnp.exp((ends[b][0] + after[b]) - within_ref[at, :lanes])).astype(BF16)
        kd_ref[at, lanes:] = (key * jnp.exp((ends[b][1] + before[b]) - within_ref[at, lanes:])).astype(BF16)
    full = tn(v_ref[...], kd_ref[...])
    mine = first_head((HEAD_V, lanes))
    for n, total in enumerate((total_f, total_b)):
        u = full[:, n * lanes : (n + 1) * lanes]
        base = n * HEAD_V
        state_ref[base : base + HEAD_V, :] = jnp.where(mine, u[:HEAD_V], u[HEAD_V:]).astype(BF16)
    tail = lax.broadcasted_iota(jnp.int32, (16, lanes), 0)
    state_ref[2 * HEAD_V :, :] = jnp.where(tail < 8, jnp.exp(total_f), jnp.exp(total_b)).astype(BF16)


def attend_kernel(
    count, place_ref, q_ref, k_ref, v_ref, within_ref, states_ref, gate_ref, gain_ref, out_ref, held_ref
):
    tokens, lanes = k_ref.shape
    blocks = tokens // BLOCK
    place = place_ref[0]
    mine = first_head((HEAD_V, lanes))
    fwd_state = jnp.zeros((HEAD_V, lanes), F32)
    bwd_state = jnp.zeros((HEAD_V, lanes), F32)
    for lap in range(count):
        memory = states_ref[lap, :HEAD_V, :].astype(F32)
        decay = states_ref[lap, 2 * HEAD_V : 2 * HEAD_V + 1, :].astype(F32)
        fwd_state = jnp.where(lap < place, fwd_state * decay + memory, fwd_state)
        other = count - 1 - lap
        memory = states_ref[other, HEAD_V : 2 * HEAD_V, :].astype(F32)
        decay = states_ref[other, 2 * HEAD_V + 8 : 2 * HEAD_V + 9, :].astype(F32)
        bwd_state = jnp.where(other > place, bwd_state * decay + memory, bwd_state)

    def spread(state):
        return jnp.concatenate([jnp.where(mine, state, 0.0), jnp.where(mine, 0.0, state)], axis=0).astype(BF16)

    def pack(u):
        return jnp.where(mine, u[:HEAD_V], u[HEAD_V:])

    for b in reversed(range(blocks)):
        at = slice(b * BLOCK, (b + 1) * BLOCK)
        held_ref[b] = spread(bwd_state)
        within = within_ref[at, lanes:]
        end = within[:1, :]
        kd = (k_ref[at, :].astype(F32) * jnp.exp(end - within)).astype(BF16)
        bwd_state = bwd_state * jnp.exp(end) + pack(tn(v_ref[at, :], kd))
    row = lax.broadcasted_iota(jnp.int32, (2 * BLOCK, BLOCK), 0) % BLOCK
    col = lax.broadcasted_iota(jnp.int32, (2 * BLOCK, BLOCK), 1)
    half = first_head((BLOCK, lanes))
    for b in range(blocks):
        at = slice(b * BLOCK, (b + 1) * BLOCK)
        query = q_ref[at, :].astype(F32) * KEY_CHANNELS ** (-0.5)
        key = k_ref[at, :].astype(F32)
        value = v_ref[at, :]
        scores, reach = [], []
        for n in range(2):
            within = within_ref[at, n * lanes : (n + 1) * lanes]
            pivot = within[BLOCK // 2 - 1 + n : BLOCK // 2 + n, :]
            near = (query * jnp.exp(within - pivot)).astype(BF16)
            far = (key * jnp.exp(pivot - within)).astype(BF16)
            zero = jnp.zeros_like(near)
            pair = jnp.concatenate([jnp.where(half, near, zero), jnp.where(half, zero, near)], axis=0)
            scores.append(nt(pair, far))
            reach.append((query * jnp.exp(within)).astype(BF16))
        score = (jnp.where(col <= row, scores[0], 0.0) + jnp.where(col >= row, scores[1], 0.0)).astype(BF16)
        states = jnp.concatenate([spread(fwd_state), held_ref[b]], axis=1)
        result = nt(jnp.concatenate(reach, axis=1), states)
        for h in range(2):
            lane = slice(h * HEAD_V, (h + 1) * HEAD_V)
            x = result[:, lane] + jnp.dot(
                score[h * BLOCK : (h + 1) * BLOCK], value[:, lane], preferred_element_type=F32
            )
            inverse = lax.rsqrt(jnp.mean(x * x, axis=-1, keepdims=True) + EPSILON)
            g = gate_ref[at, lane].astype(F32)
            out_ref[at, lane] = (x * inverse * gain_ref[:, lane] * (g * jax.nn.sigmoid(g))).astype(BF16)
        within = within_ref[at, :lanes]
        end = within[BLOCK - 1 :, :]
        kd = (key * jnp.exp(end - within)).astype(BF16)
        fwd_state = fwd_state * jnp.exp(end) + pack(tn(value, kd))


def gate_kernel(place_ref, x_ref, own_g, own_u, *refs):
    pieces, out_ref, full = refs[:-3], refs[-3], refs[-2:]
    place, side = place_ref[0], place_ref[1]
    depth = own_g.shape[0]
    part = depth // 2
    count = x_ref.shape[1] // depth
    half = len(pieces) // 2
    for n, own in enumerate((own_g, own_u)):
        full[n][pl.ds(pl.multiple_of(place * depth, depth), depth), :] = own[...]
        sources = (
            (lax.rem(place + count - 1, count), place > 0),
            (lax.rem(place + 1, count), place < count - 1),
            (lax.rem(place + 2, count), None),
            (lax.rem(place + count - 1 + 2 * (place // (count - 1)), count), (place == 0) | (place == count - 1)),
        )
        for s, (source, valid) in enumerate(sources):
            for t in range(2):
                ref = pieces[n * half + 2 * s + t]
                where = source * depth + (side if t == 0 else 1 - side) * part

                def put(ref=ref, where=where, n=n):
                    full[n][pl.ds(pl.multiple_of(where, part), part), :] = ref[...]

                if valid is None:
                    put()
                else:
                    pl.when(valid)(put)
    g = jnp.dot(x_ref[...], full[0][...], preferred_element_type=F32)
    u = jnp.dot(x_ref[...], full[1][...], preferred_element_type=F32)
    out_ref[...] = (g * jax.nn.sigmoid(g) * u).astype(BF16)


def down_kernel(place_ref, h_ref, own, *refs):
    pieces, out_ref, block = refs[:-2], refs[-2], refs[-1]
    place, side = place_ref[0], place_ref[1]
    depth, width = own.shape
    part = depth // 2
    count = out_ref.shape[1] // width
    low = pl.multiple_of(side * part, part)
    high = pl.multiple_of((1 - side) * part, part)

    def emit(source, weight):
        where = pl.ds(pl.multiple_of(source * width, width), width)
        out_ref[:, where] = jnp.dot(h_ref[...], weight, preferred_element_type=F32).astype(BF16)

    emit(place, own[...])
    for s, (source, edge) in enumerate(
        ((lax.rem(place + count - 1, count), 0), (lax.rem(place + 1, count), count - 1), (lax.rem(place + 2, count), None))
    ):

        def load(n):
            block[pl.ds(low, part), :] = pieces[2 * n][...]
            block[pl.ds(high, part), :] = pieces[2 * n + 1][...]

        if edge is None:
            load(s)
        else:
            pl.when(place != edge)(functools.partial(load, s))
            pl.when(place == edge)(functools.partial(load, 3))
        emit(source, block[...])


VMEM = pl.BlockSpec(memory_space=pltpu.VMEM)
SMEM = pl.BlockSpec(memory_space=pltpu.SMEM)


def cost(flops, size):
    return pl.CostEstimate(flops=flops, bytes_accessed=size, transcendentals=0)


def entering(value, axis, join, neutral, backward):
    count = lax.axis_size(axis)
    place = lax.axis_index(axis)
    ahead = count - 1 - place if backward else place
    gathered = jax.tree.map(
        lambda a, kind: lax.all_gather(a.astype(kind), axis), value, (jnp.bfloat16, jnp.bfloat16)
    )
    state = jax.tree.map(lambda a, e: jnp.zeros_like(a) + jnp.asarray(e, a.dtype), value, neutral)

    def one(lap, state):
        source = count - 1 - lap if backward else lap
        return join(
            state,
            jax.tree.map(
                lambda a, own: lax.dynamic_index_in_dim(a, source, 0, False).astype(own.dtype),
                gathered,
                value,
            ),
        )

    return lax.fori_loop(0, ahead, one, state)


def block_sweep(query_in, key_in, values_in, log_decay, span):
    sequence_length, head_count, key_dim = key_in.shape
    block_count = sequence_length // span

    def blocks(tensor):
        return jnp.transpose(
            tensor.reshape(block_count, span, head_count, tensor.shape[-1]), (0, 2, 1, 3)
        )

    lower_mask = jnp.tril(jnp.ones((span, span), dtype=bool))[:, :, None]

    def advance(carried, inputs):
        memory, offset = carried
        key_blk, value_blk, decay_blk, query_blk = inputs
        within = jnp.cumsum(decay_blk, axis=1)
        ending = within[:, -1, :]
        memory_next = jnp.exp(ending)[:, :, None] * memory + jnp.einsum(
            "hjd,hje->hde",
            key_blk * jnp.exp(ending[:, None, :] - within),
            value_blk,
            precision=lax.Precision.HIGHEST,
        )
        result = jnp.einsum(
            "hid,hde->hie", query_blk * jnp.exp(within), memory, precision=lax.Precision.HIGHEST
        )
        spread = jnp.exp(
            jnp.where(lower_mask, within[:, :, None, :] - within[:, None, :, :], -jnp.inf)
        )
        scores = jnp.einsum(
            "hid,hjd,hijd->hij", query_blk, key_blk, spread, precision=lax.Precision.HIGHEST
        )
        result = result + jnp.einsum(
            "hij,hje->hie", scores, value_blk, precision=lax.Precision.HIGHEST
        )
        reached = query_blk * jnp.exp(within + offset[:, None, :])
        return ((memory_next, offset + ending), (result, reached))

    start_memory = jnp.zeros((head_count, key_dim, values_in.shape[-1]), jnp.float32)
    start_offset = jnp.zeros((head_count, key_dim), jnp.float32)
    (memory, decay_total), (outputs, reached) = lax.scan(
        advance,
        (start_memory, start_offset),
        (blocks(key_in), blocks(values_in), blocks(log_decay), blocks(query_in)),
    )

    def unblock(tensor):
        return jnp.transpose(tensor, (0, 2, 1, 3)).reshape(
            sequence_length, head_count, tensor.shape[-1]
        )

    return (unblock(outputs), unblock(reached), memory, decay_total)


def head_mix(combined, head_norm_gain, output_gate_preact):
    sequence_length, head_count, width = combined.shape
    inverse = lax.rsqrt(jnp.mean(combined * combined, axis=-1, keepdims=True) + EPSILON)
    gate_act = jax.nn.silu(
        output_gate_preact.astype(jnp.float32).reshape(sequence_length, head_count, width)
    )
    weighted = combined * inverse * head_norm_gain.reshape(head_count, width) * gate_act
    return weighted.reshape(sequence_length, head_count * width).astype(jnp.bfloat16)


def row_norm(mid_rows, prenorm_gain):
    wide = mid_rows.astype(jnp.float32)
    inverse = lax.rsqrt(jnp.mean(wide * wide, axis=-1, keepdims=True) + EPSILON)
    return (wide * inverse * prenorm_gain).astype(jnp.bfloat16)


def combine_states(earlier, later):
    decay_early, memory_early = earlier
    decay_late, memory_late = later
    return (decay_early * decay_late, decay_late[:, :, None] * memory_early + memory_late)


def body(
    queries,
    key_projected,
    values,
    output_gate_preact,
    forward_decay_logits,
    backward_decay_logits,
    decay_logit_shift,
    decay_spike_values,
    residual,
    head_norm_gain,
    output_projection,
    prenorm_gain,
    gate_projection,
    up_projection,
    down_projection,
):
    sequence_length = queries.shape[0]
    local_heads = queries.shape[1] // KEY_CHANNELS
    query_f = queries.astype(jnp.float32).reshape(
        sequence_length, local_heads, KEY_CHANNELS
    ) * KEY_CHANNELS ** (-0.5)
    keys_f = key_projected.astype(jnp.float32).reshape(sequence_length, local_heads, KEY_CHANNELS)
    values_f = values.astype(jnp.float32).reshape(sequence_length, local_heads, HEAD_V)
    decay_spikes = jnp.transpose(decay_spike_values)[:, :, None]
    logit_shifts = decay_logit_shift.reshape(2, local_heads, KEY_CHANNELS)
    forward_decay = (
        jax.nn.log_sigmoid(
            forward_decay_logits.astype(jnp.float32).reshape(
                sequence_length, local_heads, KEY_CHANNELS
            )
            + logit_shifts[0]
        )
        / GATE_DENOMINATOR
        + decay_spikes
    )
    backward_decay = (
        jax.nn.log_sigmoid(
            backward_decay_logits.astype(jnp.float32).reshape(
                sequence_length, local_heads, KEY_CHANNELS
            )
            + logit_shifts[1]
        )
        / GATE_DENOMINATOR
        + decay_spikes
    )
    fwd_out, fwd_reach, fwd_memory, fwd_total = block_sweep(
        query_f, keys_f, values_f, forward_decay, BLOCK
    )
    bwd_out, bwd_reach, bwd_memory, bwd_total = block_sweep(
        query_f[::-1], keys_f[::-1], values_f[::-1], backward_decay[::-1], BLOCK
    )
    identity = (jnp.ones_like(fwd_total), jnp.zeros_like(fwd_memory))
    fwd_incoming = entering(
        (jnp.exp(fwd_total), fwd_memory), "sp", combine_states, identity, False
    )[1]
    bwd_incoming = entering((jnp.exp(bwd_total), bwd_memory), "sp", combine_states, identity, True)[
        1
    ]
    fwd_full = fwd_out + jnp.einsum(
        "lhd,hde->lhe", fwd_reach, fwd_incoming, precision=lax.Precision.HIGHEST
    )
    bwd_full = bwd_out + jnp.einsum(
        "lhd,hde->lhe", bwd_reach, bwd_incoming, precision=lax.Precision.HIGHEST
    )
    attended = head_mix(fwd_full + bwd_full[::-1], head_norm_gain, output_gate_preact)
    token_rows = lax.all_to_all(attended, "tp", split_axis=0, concat_axis=1, tiled=True)
    whole_out = lax.all_gather(output_projection, "tp", axis=0, tiled=True)
    projected = jnp.dot(token_rows, whole_out, preferred_element_type=jnp.float32)
    mid_rows = (residual.astype(jnp.float32) + projected).astype(jnp.bfloat16)
    normed = row_norm(mid_rows, prenorm_gain)
    fetched = (
        lax.all_gather(gate_projection, "sp", axis=0, tiled=True),
        lax.all_gather(up_projection, "sp", axis=0, tiled=True),
        lax.all_gather(down_projection, "sp", axis=1, tiled=True),
    )
    gate_full, up_full, down_full = fetched
    piece = lax.all_gather(normed, "tp", axis=0, tiled=True)
    gate_part = jnp.dot(piece, gate_full, preferred_element_type=jnp.float32)
    up_part = jnp.dot(piece, up_full, preferred_element_type=jnp.float32)
    hidden = (jax.nn.silu(gate_part) * up_part).astype(jnp.bfloat16)
    summed = lax.psum_scatter(
        jnp.dot(hidden, down_full, preferred_element_type=jnp.float32).astype(jnp.bfloat16),
        "tp",
        scatter_dimension=0,
        tiled=True,
    ).astype(jnp.float32)
    return (mid_rows.astype(jnp.float32) + 0.5 * summed).astype(jnp.bfloat16)


def weight_pieces(weight, axis_side):
    part = weight.shape[0] // 2
    return lax.dynamic_slice_in_dim(weight, axis_side * part, part, 0)


def line_first(half, count):
    up = lax.ppermute(half, "sp", [(i, i + 1) for i in range(count - 1)])
    down = lax.ppermute(half, "sp", [(i + 1, i) for i in range(count - 1)])
    return up, down


def line_rest(half, count):
    across = lax.ppermute(half, "sp", [(i, (i + 2) % count) for i in range(count)])
    last = lax.ppermute(across, "sp", [(2, 3), (1, 0)])
    return across, last


def swap_sides(array, groups, count, places):
    pairs = [(g * count + p, (g ^ 1) * count + p) for g in range(groups) for p in places]
    return lax.ppermute(array, ("grp", "sp"), pairs)


def fast_body(
    queries,
    key_projected,
    values,
    output_gate_preact,
    forward_decay_logits,
    backward_decay_logits,
    decay_logit_shift,
    decay_spike_values,
    residual,
    head_norm_gain,
    output_projection,
    prenorm_gain,
    gate_projection,
    up_projection,
    down_projection,
):
    count = lax.axis_size("sp")
    groups = lax.axis_size("grp")
    place = lax.axis_index("sp")
    side = lax.rem(lax.axis_index("grp"), 2)
    spot = jnp.stack([place, side]).astype(jnp.int32)
    tokens, lanes = queries.shape
    width = values.shape[1]
    rows = 2 * HEAD_V + 16

    gate_up = jnp.concatenate([weight_pieces(gate_projection, side), weight_pieces(up_projection, side)], axis=1)
    down_half = weight_pieces(down_projection, side)
    gu_up, gu_down = line_first(gate_up, count)

    within, state = pl.pallas_call(
        state_kernel,
        out_shape=(
            jax.ShapeDtypeStruct((tokens, 2 * lanes), F32),
            jax.ShapeDtypeStruct((rows, lanes), BF16),
        ),
        in_specs=[VMEM] * 6,
        out_specs=(VMEM, VMEM),
        scratch_shapes=[pltpu.VMEM((tokens, 2 * lanes), BF16)],
        cost_estimate=cost(2 * 10**9, 4 * 10**6),
        name="own_state",
    )(
        key_projected,
        values,
        forward_decay_logits,
        backward_decay_logits,
        decay_logit_shift,
        jnp.transpose(decay_spike_values),
    )
    states = lax.all_gather(state, "sp")
    states, gate_up, down_half = lax.optimization_barrier((states, gate_up, down_half))
    gu_across, gu_last = line_rest(gate_up, count)
    d_up, d_down = line_first(down_half, count)
    d_across, d_last = line_rest(down_half, count)
    inner, outer, ends = range(1, count), range(count - 1), (0, count - 1)

    def both_sides(up, down, across, last):
        found = []
        for piece, places in ((up, inner), (down, outer), (across, range(count)), (last, ends)):
            found += [piece, swap_sides(piece, groups, count, places)]
        return found

    gu_pieces = both_sides(gu_up, gu_down, gu_across, gu_last)
    d_pieces = both_sides(d_up, d_down, d_across, d_last)

    attended = pl.pallas_call(
        functools.partial(attend_kernel, count),
        out_shape=jax.ShapeDtypeStruct((tokens, width), BF16),
        in_specs=[SMEM] + [VMEM] * 7,
        out_specs=VMEM,
        scratch_shapes=[pltpu.VMEM((tokens // BLOCK, 2 * HEAD_V, lanes), BF16)],
        cost_estimate=cost(10**10, 8 * 10**6),
        name="attend",
    )(
        spot,
        queries,
        key_projected,
        values,
        within,
        states,
        output_gate_preact,
        head_norm_gain[None, :],
    )
    whole_out = lax.all_gather(output_projection, "tp", axis=0, tiled=True)
    whole_residual = lax.all_gather(residual, "tp", axis=0, tiled=True)
    token_rows = lax.all_gather(attended, "tp", axis=1, tiled=True)
    projected = jnp.dot(token_rows, whole_out, preferred_element_type=F32)
    mid = (whole_residual.astype(F32) + projected).astype(BF16)
    normed = row_norm(mid, prenorm_gain)

    model = normed.shape[1]
    depth, hidden_width = gate_projection.shape
    tile = 256 if hidden_width % 256 == 0 else hidden_width
    steps = hidden_width // tile
    column = lambda size, first: pl.BlockSpec((size, tile), lambda j: (0, j + first))
    hidden = pl.pallas_call(
        gate_kernel,
        grid=(steps,),
        out_shape=jax.ShapeDtypeStruct((tokens, hidden_width), BF16),
        in_specs=[SMEM, pl.BlockSpec((tokens, model), lambda j: (0, 0))]
        + [column(depth, 0)] * 2
        + [column(depth // 2, 0)] * 8
        + [column(depth // 2, steps)] * 8,
        out_specs=column(tokens, 0),
        scratch_shapes=[pltpu.VMEM((model, tile), BF16)] * 2,
        cost_estimate=cost(4 * tokens * model * hidden_width, 4 * model * hidden_width),
        name="gate_up",
    )(spot, normed, gate_projection, up_projection, *gu_pieces, *gu_pieces)
    partial = pl.pallas_call(
        down_kernel,
        out_shape=jax.ShapeDtypeStruct((tokens, model), BF16),
        in_specs=[SMEM] + [VMEM] * 10,
        out_specs=VMEM,
        scratch_shapes=[pltpu.VMEM(down_projection.shape, BF16)],
        cost_estimate=cost(2 * tokens * model * hidden_width, 2 * model * hidden_width),
        name="down",
    )(spot, hidden, down_projection, *d_pieces)
    summed = lax.psum_scatter(partial, "tp", scatter_dimension=0, tiled=True).astype(F32)
    own = residual.shape[0]
    mid_rows = lax.dynamic_slice_in_dim(mid, lax.axis_index("tp") * own, own, 0)
    return (mid_rows.astype(F32) + 0.5 * summed).astype(BF16)


def solution(mesh):
    in_specs = (
        P(("grp", "sp"), "tp"),
        P(("grp", "sp"), "tp"),
        P(("grp", "sp"), "tp"),
        P(("grp", "sp"), "tp"),
        P(("grp", "sp"), "tp"),
        P(("grp", "sp"), "tp"),
        P(None, "tp"),
        P("tp", ("grp", "sp")),
        P(("grp", "sp", "tp"), None),
        P("tp"),
        P("tp", None),
        P(),
        P("sp", "tp"),
        P("sp", "tp"),
        P("tp", "sp"),
    )
    out_specs = P(("grp", "sp", "tp"), None)

    def run(*args):
        lanes = args[0].shape[1]
        fits = lanes == 2 * KEY_CHANNELS and mesh.shape["sp"] == 4 and mesh.shape["grp"] % 2 == 0
        return (fast_body if fits else body)(*args)

    return jax.shard_map(run, mesh=mesh, in_specs=in_specs, out_specs=out_specs, check_vma=False)
```

```python
import functools

import jax
import jax.numpy as jnp
from jax import lax
from jax.experimental import pallas as pl
from jax.experimental.pallas import tpu as pltpu
from jax.sharding import PartitionSpec as P


KEY_CHANNELS = 64
HEAD_V = 128
BLOCK = 64
GATE_DENOMINATOR = 16.0
EPSILON = 1e-06
F32, BF16 = jnp.float32, jnp.bfloat16


def nt(a, b):
    return lax.dot_general(a, b, (((1,), (1,)), ((), ())), preferred_element_type=F32)


def tn(a, b):
    return lax.dot_general(a, b, (((0,), (0,)), ((), ())), preferred_element_type=F32)


def first_head(shape):
    return lax.broadcasted_iota(jnp.int32, shape, 1) < KEY_CHANNELS


def state_kernel(k_ref, v_ref, fd_ref, bd_ref, shift_ref, spike_ref, within_ref, state_ref, kd_ref):
    tokens, lanes = k_ref.shape
    blocks = tokens // BLOCK
    row = lax.broadcasted_iota(jnp.int32, (2 * BLOCK, 2 * BLOCK), 0)
    col = lax.broadcasted_iota(jnp.int32, (2 * BLOCK, 2 * BLOCK), 1)
    r, c = row % BLOCK, col % BLOCK
    ahead = jnp.where(row < BLOCK, r - c, c - r)
    tri = jnp.where(ahead >= 0, 1.0, 0.0).astype(BF16)
    half = first_head((BLOCK, lanes))
    ends = []
    for b in range(blocks):
        at = slice(b * BLOCK, (b + 1) * BLOCK)
        spike = jnp.where(half, spike_ref[at, 0:1], spike_ref[at, 1:2])
        parts = []
        for n, ref in enumerate((fd_ref, bd_ref)):
            x = ref[at, :].astype(F32) + shift_ref[n : n + 1, :]
            soft = jnp.minimum(x, 0.0) - jnp.log1p(jnp.exp(-jnp.abs(x)))
            parts.append(soft / GATE_DENOMINATOR + spike)
        d = jnp.concatenate(parts, axis=1)
        hi = d.astype(BF16)
        lo = (d - hi.astype(F32)).astype(BF16)
        both = jnp.dot(tri, jnp.concatenate([hi, lo], axis=0), preferred_element_type=F32)
        fwd, bwd = both[:BLOCK, :lanes], both[BLOCK:, lanes:]
        within_ref[at, :lanes] = fwd
        within_ref[at, lanes:] = bwd
        ends.append((fwd[BLOCK - 1 :, :], bwd[:1, :]))
    zero = jnp.zeros((1, lanes), F32)
    after, before = [zero] * blocks, [zero] * blocks
    for b in range(1, blocks):
        before[b] = before[b - 1] + ends[b - 1][1]
        after[blocks - 1 - b] = after[blocks - b] + ends[blocks - b][0]
    total_f, total_b = after[0] + ends[0][0], before[-1] + ends[-1][1]
    for b in range(blocks):
        at = slice(b * BLOCK, (b + 1) * BLOCK)
        key = k_ref[at, :].astype(F32)
        kd_ref[at, :lanes] = (key * jnp.exp((ends[b][0] + after[b]) - within_ref[at, :lanes])).astype(BF16)
        kd_ref[at, lanes:] = (key * jnp.exp((ends[b][1] + before[b]) - within_ref[at, lanes:])).astype(BF16)
    full = tn(v_ref[...], kd_ref[...])
    mine = first_head((HEAD_V, lanes))
    for n, total in enumerate((total_f, total_b)):
        u = full[:, n * lanes : (n + 1) * lanes]
        base = n * HEAD_V
        state_ref[base : base + HEAD_V, :] = jnp.where(mine, u[:HEAD_V], u[HEAD_V:]).astype(BF16)
    tail = lax.broadcasted_iota(jnp.int32, (16, lanes), 0)
    state_ref[2 * HEAD_V :, :] = jnp.where(tail < 8, jnp.exp(total_f), jnp.exp(total_b)).astype(BF16)


def attend_kernel(
    count, place_ref, q_ref, k_ref, v_ref, within_ref, gate_ref, gain_ref, *refs
):
    states_ref, (out_ref, held_ref) = refs[:-2], refs[-2:]
    tokens, lanes = k_ref.shape
    blocks = tokens // BLOCK
    place = place_ref[0]
    mine = first_head((HEAD_V, lanes))
    fwd_state = jnp.zeros((HEAD_V, lanes), F32)
    bwd_state = jnp.zeros((HEAD_V, lanes), F32)
    for k in reversed(range(1, count)):
        before, after = states_ref[k - 1], states_ref[count - k - 1]
        memory = before[:HEAD_V, :].astype(F32)
        decay = before[2 * HEAD_V : 2 * HEAD_V + 1, :].astype(F32)
        fwd_state = jnp.where(place >= k, fwd_state * decay + memory, fwd_state)
        memory = after[HEAD_V : 2 * HEAD_V, :].astype(F32)
        decay = after[2 * HEAD_V + 8 : 2 * HEAD_V + 9, :].astype(F32)
        bwd_state = jnp.where(place + k < count, bwd_state * decay + memory, bwd_state)

    def spread(state):
        return jnp.concatenate([jnp.where(mine, state, 0.0), jnp.where(mine, 0.0, state)], axis=0).astype(BF16)

    def pack(u):
        return jnp.where(mine, u[:HEAD_V], u[HEAD_V:])

    for b in reversed(range(blocks)):
        at = slice(b * BLOCK, (b + 1) * BLOCK)
        held_ref[b] = spread(bwd_state)
        within = within_ref[at, lanes:]
        end = within[:1, :]
        kd = (k_ref[at, :].astype(F32) * jnp.exp(end - within)).astype(BF16)
        bwd_state = bwd_state * jnp.exp(end) + pack(tn(v_ref[at, :], kd))
    row = lax.broadcasted_iota(jnp.int32, (2 * BLOCK, BLOCK), 0) % BLOCK
    col = lax.broadcasted_iota(jnp.int32, (2 * BLOCK, BLOCK), 1)
    half = first_head((BLOCK, lanes))
    for b in range(blocks):
        at = slice(b * BLOCK, (b + 1) * BLOCK)
        query = q_ref[at, :].astype(F32) * KEY_CHANNELS ** (-0.5)
        key = k_ref[at, :].astype(F32)
        value = v_ref[at, :]
        scores, reach = [], []
        for n in range(2):
            within = within_ref[at, n * lanes : (n + 1) * lanes]
            pivot = within[BLOCK // 2 - 1 + n : BLOCK // 2 + n, :]
            near = (query * jnp.exp(within - pivot)).astype(BF16)
            far = (key * jnp.exp(pivot - within)).astype(BF16)
            zero = jnp.zeros_like(near)
            pair = jnp.concatenate([jnp.where(half, near, zero), jnp.where(half, zero, near)], axis=0)
            scores.append(nt(pair, far))
            reach.append((query * jnp.exp(within)).astype(BF16))
        score = (jnp.where(col <= row, scores[0], 0.0) + jnp.where(col >= row, scores[1], 0.0)).astype(BF16)
        states = jnp.concatenate([spread(fwd_state), held_ref[b]], axis=1)
        result = nt(jnp.concatenate(reach, axis=1), states)
        for h in range(2):
            lane = slice(h * HEAD_V, (h + 1) * HEAD_V)
            x = result[:, lane] + jnp.dot(
                score[h * BLOCK : (h + 1) * BLOCK], value[:, lane], preferred_element_type=F32
            )
            inverse = lax.rsqrt(jnp.mean(x * x, axis=-1, keepdims=True) + EPSILON)
            g = gate_ref[at, lane].astype(F32)
            out_ref[at, lane] = (x * inverse * gain_ref[:, lane] * (g * jax.nn.sigmoid(g))).astype(BF16)
        within = within_ref[at, :lanes]
        end = within[BLOCK - 1 :, :]
        kd = (key * jnp.exp(end - within)).astype(BF16)
        fwd_state = fwd_state * jnp.exp(end) + pack(tn(value, kd))


def gate_kernel(place_ref, x_ref, own_g, own_u, *refs):
    pieces, out_ref, full = refs[:-3], refs[-3], refs[-2:]
    place, side = place_ref[0], place_ref[1]
    depth = own_g.shape[0]
    part = depth // 2
    count = x_ref.shape[1] // depth
    half = len(pieces) // 2
    for n, own in enumerate((own_g, own_u)):
        full[n][pl.ds(pl.multiple_of(place * depth, depth), depth), :] = own[...]
        sources = []
        for k in range(1, count):
            sources += [(place - k, place >= k), (place + k, place + k < count)]
        for s, (source, valid) in enumerate(sources):
            for t in range(2):
                ref = pieces[n * half + 2 * s + t]
                where = source * depth + (side if t == 0 else 1 - side) * part

                @pl.when(valid)
                def _(ref=ref, where=where, n=n):
                    full[n][pl.ds(pl.multiple_of(where, part), part), :] = ref[...]

    g = jnp.dot(x_ref[...], full[0][...], preferred_element_type=F32)
    u = jnp.dot(x_ref[...], full[1][...], preferred_element_type=F32)
    out_ref[...] = (g * jax.nn.sigmoid(g) * u).astype(BF16)


def down_kernel(place_ref, h_ref, own, *refs):
    pieces, out_ref, block = refs[:-2], refs[-2], refs[-1]
    place, side = place_ref[0], place_ref[1]
    depth, width = own.shape
    part = depth // 2
    count = out_ref.shape[1] // width
    low = pl.multiple_of(side * part, part)
    high = pl.multiple_of((1 - side) * part, part)

    lines = out_ref.shape[0]
    taken = pl.ds(pl.multiple_of(place_ref[2] * lines, lines), lines)

    def emit(source, weight):
        where = pl.ds(pl.multiple_of(source * width, width), width)
        out_ref[:, where] = jnp.dot(h_ref[taken, :], weight, preferred_element_type=F32).astype(BF16)

    emit(place, own[...])
    sources = []
    for k in range(1, count):
        sources += [(place - k, place >= k), (place + k, place + k < count)]
    for s, (source, valid) in enumerate(sources):

        @pl.when(valid)
        def _(s=s, source=source):
            block[pl.ds(low, part), :] = pieces[2 * s][...]
            block[pl.ds(high, part), :] = pieces[2 * s + 1][...]
            emit(source, block[...])


VMEM = pl.BlockSpec(memory_space=pltpu.VMEM)
SMEM = pl.BlockSpec(memory_space=pltpu.SMEM)


def cost(flops, size):
    return pl.CostEstimate(flops=flops, bytes_accessed=size, transcendentals=0)


def entering(value, axis, join, neutral, backward):
    count = lax.axis_size(axis)
    place = lax.axis_index(axis)
    ahead = count - 1 - place if backward else place
    gathered = jax.tree.map(
        lambda a, kind: lax.all_gather(a.astype(kind), axis), value, (jnp.bfloat16, jnp.bfloat16)
    )
    state = jax.tree.map(lambda a, e: jnp.zeros_like(a) + jnp.asarray(e, a.dtype), value, neutral)

    def one(lap, state):
        source = count - 1 - lap if backward else lap
        return join(
            state,
            jax.tree.map(
                lambda a, own: lax.dynamic_index_in_dim(a, source, 0, False).astype(own.dtype),
                gathered,
                value,
            ),
        )

    return lax.fori_loop(0, ahead, one, state)


def block_sweep(query_in, key_in, values_in, log_decay, span):
    sequence_length, head_count, key_dim = key_in.shape
    block_count = sequence_length // span

    def blocks(tensor):
        return jnp.transpose(
            tensor.reshape(block_count, span, head_count, tensor.shape[-1]), (0, 2, 1, 3)
        )

    lower_mask = jnp.tril(jnp.ones((span, span), dtype=bool))[:, :, None]

    def advance(carried, inputs):
        memory, offset = carried
        key_blk, value_blk, decay_blk, query_blk = inputs
        within = jnp.cumsum(decay_blk, axis=1)
        ending = within[:, -1, :]
        memory_next = jnp.exp(ending)[:, :, None] * memory + jnp.einsum(
            "hjd,hje->hde",
            key_blk * jnp.exp(ending[:, None, :] - within),
            value_blk,
            precision=lax.Precision.HIGHEST,
        )
        result = jnp.einsum(
            "hid,hde->hie", query_blk * jnp.exp(within), memory, precision=lax.Precision.HIGHEST
        )
        spread = jnp.exp(
            jnp.where(lower_mask, within[:, :, None, :] - within[:, None, :, :], -jnp.inf)
        )
        scores = jnp.einsum(
            "hid,hjd,hijd->hij", query_blk, key_blk, spread, precision=lax.Precision.HIGHEST
        )
        result = result + jnp.einsum(
            "hij,hje->hie", scores, value_blk, precision=lax.Precision.HIGHEST
        )
        reached = query_blk * jnp.exp(within + offset[:, None, :])
        return ((memory_next, offset + ending), (result, reached))

    start_memory = jnp.zeros((head_count, key_dim, values_in.shape[-1]), jnp.float32)
    start_offset = jnp.zeros((head_count, key_dim), jnp.float32)
    (memory, decay_total), (outputs, reached) = lax.scan(
        advance,
        (start_memory, start_offset),
        (blocks(key_in), blocks(values_in), blocks(log_decay), blocks(query_in)),
    )

    def unblock(tensor):
        return jnp.transpose(tensor, (0, 2, 1, 3)).reshape(
            sequence_length, head_count, tensor.shape[-1]
        )

    return (unblock(outputs), unblock(reached), memory, decay_total)


def head_mix(combined, head_norm_gain, output_gate_preact):
    sequence_length, head_count, width = combined.shape
    inverse = lax.rsqrt(jnp.mean(combined * combined, axis=-1, keepdims=True) + EPSILON)
    gate_act = jax.nn.silu(
        output_gate_preact.astype(jnp.float32).reshape(sequence_length, head_count, width)
    )
    weighted = combined * inverse * head_norm_gain.reshape(head_count, width) * gate_act
    return weighted.reshape(sequence_length, head_count * width).astype(jnp.bfloat16)


def row_norm(mid_rows, prenorm_gain):
    wide = mid_rows.astype(jnp.float32)
    inverse = lax.rsqrt(jnp.mean(wide * wide, axis=-1, keepdims=True) + EPSILON)
    return (wide * inverse * prenorm_gain).astype(jnp.bfloat16)


def combine_states(earlier, later):
    decay_early, memory_early = earlier
    decay_late, memory_late = later
    return (decay_early * decay_late, decay_late[:, :, None] * memory_early + memory_late)


def body(
    queries,
    key_projected,
    values,
    output_gate_preact,
    forward_decay_logits,
    backward_decay_logits,
    decay_logit_shift,
    decay_spike_values,
    residual,
    head_norm_gain,
    output_projection,
    prenorm_gain,
    gate_projection,
    up_projection,
    down_projection,
):
    sequence_length = queries.shape[0]
    local_heads = queries.shape[1] // KEY_CHANNELS
    query_f = queries.astype(jnp.float32).reshape(
        sequence_length, local_heads, KEY_CHANNELS
    ) * KEY_CHANNELS ** (-0.5)
    keys_f = key_projected.astype(jnp.float32).reshape(sequence_length, local_heads, KEY_CHANNELS)
    values_f = values.astype(jnp.float32).reshape(sequence_length, local_heads, HEAD_V)
    decay_spikes = jnp.transpose(decay_spike_values)[:, :, None]
    logit_shifts = decay_logit_shift.reshape(2, local_heads, KEY_CHANNELS)
    forward_decay = (
        jax.nn.log_sigmoid(
            forward_decay_logits.astype(jnp.float32).reshape(
                sequence_length, local_heads, KEY_CHANNELS
            )
            + logit_shifts[0]
        )
        / GATE_DENOMINATOR
        + decay_spikes
    )
    backward_decay = (
        jax.nn.log_sigmoid(
            backward_decay_logits.astype(jnp.float32).reshape(
                sequence_length, local_heads, KEY_CHANNELS
            )
            + logit_shifts[1]
        )
        / GATE_DENOMINATOR
        + decay_spikes
    )
    fwd_out, fwd_reach, fwd_memory, fwd_total = block_sweep(
        query_f, keys_f, values_f, forward_decay, BLOCK
    )
    bwd_out, bwd_reach, bwd_memory, bwd_total = block_sweep(
        query_f[::-1], keys_f[::-1], values_f[::-1], backward_decay[::-1], BLOCK
    )
    identity = (jnp.ones_like(fwd_total), jnp.zeros_like(fwd_memory))
    fwd_incoming = entering(
        (jnp.exp(fwd_total), fwd_memory), "sp", combine_states, identity, False
    )[1]
    bwd_incoming = entering((jnp.exp(bwd_total), bwd_memory), "sp", combine_states, identity, True)[
        1
    ]
    fwd_full = fwd_out + jnp.einsum(
        "lhd,hde->lhe", fwd_reach, fwd_incoming, precision=lax.Precision.HIGHEST
    )
    bwd_full = bwd_out + jnp.einsum(
        "lhd,hde->lhe", bwd_reach, bwd_incoming, precision=lax.Precision.HIGHEST
    )
    attended = head_mix(fwd_full + bwd_full[::-1], head_norm_gain, output_gate_preact)
    token_rows = lax.all_to_all(attended, "tp", split_axis=0, concat_axis=1, tiled=True)
    whole_out = lax.all_gather(output_projection, "tp", axis=0, tiled=True)
    projected = jnp.dot(token_rows, whole_out, preferred_element_type=jnp.float32)
    mid_rows = (residual.astype(jnp.float32) + projected).astype(jnp.bfloat16)
    normed = row_norm(mid_rows, prenorm_gain)
    fetched = (
        lax.all_gather(gate_projection, "sp", axis=0, tiled=True),
        lax.all_gather(up_projection, "sp", axis=0, tiled=True),
        lax.all_gather(down_projection, "sp", axis=1, tiled=True),
    )
    gate_full, up_full, down_full = fetched
    piece = lax.all_gather(normed, "tp", axis=0, tiled=True)
    gate_part = jnp.dot(piece, gate_full, preferred_element_type=jnp.float32)
    up_part = jnp.dot(piece, up_full, preferred_element_type=jnp.float32)
    hidden = (jax.nn.silu(gate_part) * up_part).astype(jnp.bfloat16)
    summed = lax.psum_scatter(
        jnp.dot(hidden, down_full, preferred_element_type=jnp.float32).astype(jnp.bfloat16),
        "tp",
        scatter_dimension=0,
        tiled=True,
    ).astype(jnp.float32)
    return (mid_rows.astype(jnp.float32) + 0.5 * summed).astype(jnp.bfloat16)


def weight_pieces(weight, axis_side):
    part = weight.shape[0] // 2
    return lax.dynamic_slice_in_dim(weight, axis_side * part, part, 0)


def line_chain(half, count):
    pieces, up, down = [], half, half
    for k in range(1, count):
        up = lax.ppermute(up, "sp", [(i, i + 1) for i in range(k - 1, count - 1)])
        down = lax.ppermute(down, "sp", [(i + 1, i) for i in range(count - k)])
        pieces.append((up, down))
    return pieces


def swap_sides(array, groups, count, places):
    pairs = [(g * count + p, (g ^ 1) * count + p) for g in range(groups) for p in places]
    return lax.ppermute(array, ("grp", "sp"), pairs)


def fast_body(
    queries,
    key_projected,
    values,
    output_gate_preact,
    forward_decay_logits,
    backward_decay_logits,
    decay_logit_shift,
    decay_spike_values,
    residual,
    head_norm_gain,
    output_projection,
    prenorm_gain,
    gate_projection,
    up_projection,
    down_projection,
):
    count = lax.axis_size("sp")
    groups = lax.axis_size("grp")
    place = lax.axis_index("sp")
    side = lax.rem(lax.axis_index("grp"), 2)
    spot = jnp.stack([place, side]).astype(jnp.int32)
    tokens, lanes = queries.shape
    width = values.shape[1]
    rows = 2 * HEAD_V + 16

    gate_up = jnp.concatenate([weight_pieces(gate_projection, side), weight_pieces(up_projection, side)], axis=1)
    down_half = weight_pieces(down_projection, side)

    def spread_weights(half):
        found = []
        for k, (up, down) in enumerate(line_chain(half, count), 1):
            for piece, places in ((up, range(k, count)), (down, range(count - k))):
                found += [piece, swap_sides(piece, groups, count, places)]
        return found

    gu_pieces = spread_weights(gate_up)
    d_pieces = spread_weights(down_half)

    within, state = pl.pallas_call(
        state_kernel,
        out_shape=(
            jax.ShapeDtypeStruct((tokens, 2 * lanes), F32),
            jax.ShapeDtypeStruct((rows, lanes), BF16),
        ),
        in_specs=[VMEM] * 6,
        out_specs=(VMEM, VMEM),
        scratch_shapes=[pltpu.VMEM((tokens, 2 * lanes), BF16)],
        cost_estimate=cost(2 * 10**9, 4 * 10**6),
        name="own_state",
    )(
        key_projected,
        values,
        forward_decay_logits,
        backward_decay_logits,
        decay_logit_shift,
        jnp.transpose(decay_spike_values),
    )
    states = []
    for k in range(1, count):
        states.append(lax.ppermute(state, "sp", [(i, (i + k) % count) for i in range(count)]))
    attended = pl.pallas_call(
        functools.partial(attend_kernel, count),
        out_shape=jax.ShapeDtypeStruct((tokens, width), BF16),
        in_specs=[SMEM] + [VMEM] * (6 + len(states)),
        out_specs=VMEM,
        scratch_shapes=[pltpu.VMEM((tokens // BLOCK, 2 * HEAD_V, lanes), BF16)],
        cost_estimate=cost(10**10, 8 * 10**6),
        name="attend",
    )(
        spot,
        queries,
        key_projected,
        values,
        within,
        output_gate_preact,
        head_norm_gain[None, :],
        *states,
    )
    whole_out = lax.all_gather(output_projection, "tp", axis=0, tiled=True)
    whole_residual = lax.all_gather(residual, "tp", axis=0, tiled=True)
    token_rows = lax.all_gather(attended, "tp", axis=1, tiled=True)
    projected = jnp.dot(token_rows, whole_out, preferred_element_type=F32)
    mid = (whole_residual.astype(F32) + projected).astype(BF16)
    normed = row_norm(mid, prenorm_gain)

    model = normed.shape[1]
    depth, hidden_width = gate_projection.shape
    tile = 256 if hidden_width % 256 == 0 else hidden_width
    steps = hidden_width // tile
    column = lambda size, first: pl.BlockSpec((size, tile), lambda j: (0, j + first))
    hidden = pl.pallas_call(
        gate_kernel,
        grid=(steps,),
        out_shape=jax.ShapeDtypeStruct((tokens, hidden_width), BF16),
        in_specs=[SMEM, pl.BlockSpec((tokens, model), lambda j: (0, 0))]
        + [column(depth, 0)] * 2
        + [column(depth // 2, 0)] * len(gu_pieces)
        + [column(depth // 2, steps)] * len(gu_pieces),
        out_specs=column(tokens, 0),
        scratch_shapes=[pltpu.VMEM((model, tile), BF16)] * 2,
        cost_estimate=cost(4 * tokens * model * hidden_width, 4 * model * hidden_width),
        name="gate_up",
    )(spot, normed, gate_projection, up_projection, *gu_pieces, *gu_pieces)
    mesh_place = lax.axis_index("tp")
    chip, core = mesh_place // 2, lax.rem(mesh_place, 2)
    chips = lax.axis_size("tp") // 2
    lines = tokens // chips

    def partial(which):
        return pl.pallas_call(
            down_kernel,
            out_shape=jax.ShapeDtypeStruct((lines, model), BF16),
            in_specs=[SMEM] + [VMEM] * (2 + len(d_pieces)),
            out_specs=VMEM,
            scratch_shapes=[pltpu.VMEM(down_projection.shape, BF16)],
            cost_estimate=cost(2 * lines * model * hidden_width, 2 * model * hidden_width),
        )(jnp.stack([place, side, which]).astype(jnp.int32), hidden, down_projection, *d_pieces)

    own = residual.shape[0]

    def core_sum(array):
        keep = lax.dynamic_slice_in_dim(array, core * own, own, 0)
        give = lax.dynamic_slice_in_dim(array, (1 - core) * own, own, 0)
        got = lax.ppermute(give, "tp", [(i, i ^ 1) for i in range(2 * chips)])
        return keep.astype(F32) + got.astype(F32)

    far = core_sum(partial(1 - chip)).astype(BF16)
    far = lax.ppermute(far, "tp", [(i, i ^ 2) for i in range(2 * chips)])
    near = core_sum(partial(chip))
    summed = near + far.astype(F32)
    mid_rows = lax.dynamic_slice_in_dim(mid, mesh_place * own, own, 0)
    return (mid_rows.astype(F32) + 0.5 * summed).astype(BF16)


def solution(mesh):
    in_specs = (
        P(("grp", "sp"), "tp"),
        P(("grp", "sp"), "tp"),
        P(("grp", "sp"), "tp"),
        P(("grp", "sp"), "tp"),
        P(("grp", "sp"), "tp"),
        P(("grp", "sp"), "tp"),
        P(None, "tp"),
        P("tp", ("grp", "sp")),
        P(("grp", "sp", "tp"), None),
        P("tp"),
        P("tp", None),
        P(),
        P("sp", "tp"),
        P("sp", "tp"),
        P("tp", "sp"),
    )
    out_specs = P(("grp", "sp", "tp"), None)

    def run(*args):
        lanes = args[0].shape[1]
        fits = lanes == 2 * KEY_CHANNELS and mesh.shape["sp"] == 4 and mesh.shape["grp"] % 2 == 0 and mesh.shape["tp"] == 4
        if not fits:
            return body(*args)
        return fast_body(*args)

    return jax.shard_map(run, mesh=mesh, in_specs=in_specs, out_specs=out_specs, check_vma=False)
```
